32 devices in a mesh: sp: 8 (over z, y), tp: 4 (over x, core).
Axes of the slice: x: 2, y: 2, z: 4, core: 2. Of those that a mesh axis runs over, the one named last changes fastest.
Arguments:
- tokens: bfloat16 [4096, 2048], P(('sp', 'tp')), may hold values from -6 to 6
- input_gain: float32 [2048], replicated, may hold values from 0.1 to 1.9
- recur_query: bfloat16 [2048, 2048], P(None, 'tp'), may hold values from -0.125 to 0.125
- recur_forget: bfloat16 [2048, 2048], P(None, 'tp'), may hold values from -0.125 to 0.125
- recur_input: bfloat16 [2048, 1024], P(None, 'tp'), may hold values from -0.125 to 0.125
- recur_gate: bfloat16 [2048, 1024], P(None, 'tp'), may hold values from -0.125 to 0.125
- first_query: bfloat16 [2048, 512], P(None, 'tp'), may hold values from -0.18782524 to 0.18782524
- second_query: bfloat16 [2048, 512], P(None, 'tp'), may hold values from -0.18782524 to 0.18782524
- first_key: bfloat16 [2048, 512], P(None, 'tp'), may hold values from -5.7452426 to 5.7452426
- second_key: bfloat16 [2048, 512], P(None, 'tp'), may hold values from -5.7452426 to 5.7452426
- diff_value: bfloat16 [2048, 1024], P(None, 'tp'), may hold values from -0.125 to 0.125
- forget_floor: float32 [16, 128], P('tp'), may hold values from 9.765625e-05 to 0.08
- decay_shift: float32 [16, 4096], P('tp', 'sp'), may hold values from -0.7 to 0
- recur_gain: float32 [64], replicated, may hold values from 0.1 to 1.9
- diff_gain: float32 [64], replicated, may hold values from 0.1 to 1.9
- diff_lambda: float32 [16], P('tp'), may hold values from 0.3 to 0.8
- recur_out: bfloat16 [1024, 2048], P('tp'), may hold values from -0.125 to 0.125
- diff_out: bfloat16 [1024, 2048], P('tp'), may hold values from -0.125 to 0.125
- final_gain: float32 [2048], replicated, may hold values from 0.1 to 1.9
Outputs:
- layer_out: bfloat16 [4096, 2048], P(('sp', 'tp'))
- row_logsum: float32 [2, 16, 4096], P(None, 'tp', 'sp')
The draws below stay inside these ranges and needn't reach their ends.
All inputs are finite; a program needn't handle non-finite values.
Results may differ from the reference program's by a relative error of at most 0.014.
Values may be sent and summed in bfloat16 or wider, within the bound.
A program may use at most 128 MiB of HBM per device.

```python
import math
import jax
import jax.numpy as jnp
from jax import lax

D = 2048
HEADS = 16
HEAD = 64
STATE_K = 128
QK = 32
SPAN = 64
TOK_DEV = 512
TOKENS = 4096


def diff_pairs(key):
    keys = jax.random.split(jax.random.fold_in(key, 7), 4)
    scale = 1.4 / math.sqrt(D)

    def normal_part(subkey):
        return jnp.clip(jax.random.normal(subkey, (D, HEADS * QK), jnp.float32), -6.0, 6.0) * scale
    query_one = normal_part(keys[0])
    query_two = normal_part(keys[1])
    key_one = normal_part(keys[2])
    key_two = normal_part(keys[3])
    return (query_one, query_two, key_one, key_two)


def draw_first_query(key, part):
    return diff_pairs(key)[0].astype(jnp.bfloat16)


def draw_second_query(key, part):
    return diff_pairs(key)[1].astype(jnp.bfloat16)


def draw_first_key(key, part):
    return diff_pairs(key)[2].astype(jnp.bfloat16)


def draw_second_key(key, part):
    return diff_pairs(key)[3].astype(jnp.bfloat16)


def draw_forget_floor(key, part):
    keys = jax.random.split(jax.random.fold_in(key, 11), 3)
    share = 0.5
    slow = jax.random.uniform(keys[0], (HEADS, 1), jnp.float32) < share
    slow_gap = jnp.exp(jax.random.uniform(keys[1], (HEADS, STATE_K), jnp.float32, math.log(0.4), math.log(1.2))) / TOKENS
    fast_gap = jnp.exp(jax.random.uniform(keys[2], (HEADS, STATE_K), jnp.float32, math.log(0.03), math.log(0.08)))
    return jnp.where(slow, slow_gap, fast_gap)


def draw_decay_shift(key, part):
    keys = jax.random.split(jax.random.fold_in(key, 13), 3)
    blocks = TOKENS // TOK_DEV
    rate = jnp.exp(jax.random.uniform(keys[0], (HEADS, blocks), jnp.float32, math.log(0.2), math.log(0.6))) / TOKENS
    steady_state = -jnp.repeat(rate, TOK_DEV, axis=1)
    position_index = jax.random.randint(keys[1], (HEADS, 2), 0, TOKENS)
    layer_depth = jnp.log(jax.random.uniform(keys[2], (HEADS, 2), jnp.float32, 0.55, 0.8))
    token_positions = jnp.arange(TOKENS)
    token_groups = jnp.sum(jnp.where(token_positions[None, None, :] == position_index[:, :, None], layer_depth[:, :, None], 0.0), axis=1)
    return steady_state + token_groups


def levels(rng, extent, cuts, smallest, largest):
    loudness = 1.0
    for axis_at, shards_of in cuts:
        draws = jax.random.uniform(jax.random.fold_in(jax.random.fold_in(rng, 6), axis_at), (shards_of,), jnp.float32, smallest / len(cuts), largest / len(cuts))
        loudness = loudness * jnp.repeat(jnp.exp(draws), extent[axis_at] // shards_of).reshape((-1,) + (1,) * (len(extent) - 1 - axis_at))
    return loudness


def normal_values(stream_key, extent, deviation, most, cuts=(), kind=jnp.bfloat16):
    values = jax.random.normal(stream_key, extent, jnp.float32) * deviation
    if len(cuts) > 0:
        values = levels(stream_key, extent, cuts, -0.22, 0.18) * values
    return jnp.clip(values, min=-most, max=most).astype(kind)


def setup_inputs(seed: int = 0) -> dict:
    seeds = jax.random.split(jax.random.key(seed), 20)
    tokens = normal_values(seeds[0], (TOKENS, D), 1.0, 6.0, ((0, 32),))
    input_gain = jnp.clip(1.0 + 0.18 * jax.random.normal(seeds[1], (D,), jnp.float32), 0.1, 1.9)
    recur_query = normal_values(seeds[2], (D, HEADS * STATE_K), D ** -0.5, 0.125, ((1, 4),))
    recur_forget = normal_values(seeds[3], (D, HEADS * STATE_K), D ** -0.5, 0.125, ((1, 4),))
    recur_input = normal_values(seeds[4], (D, HEADS * HEAD), D ** -0.5, 0.125, ((1, 4),))
    recur_gate = normal_values(seeds[5], (D, HEADS * HEAD), D ** -0.5, 0.125, ((1, 4),))
    first_query = draw_first_query(jax.random.fold_in(seeds[19], 71), 0)
    second_query = draw_second_query(jax.random.fold_in(seeds[19], 71), 0)
    first_key = draw_first_key(jax.random.fold_in(seeds[19], 71), 0)
    second_key = draw_second_key(jax.random.fold_in(seeds[19], 71), 0)
    diff_value = normal_values(seeds[10], (D, HEADS * HEAD), D ** -0.5, 0.125, ((1, 4),))
    forget_floor = draw_forget_floor(jax.random.fold_in(seeds[19], 71), 0)
    decay_shift = draw_decay_shift(jax.random.fold_in(seeds[19], 71), 0)
    recur_gain = jnp.clip(1.0 + 0.18 * jax.random.normal(seeds[13], (HEAD,), jnp.float32), 0.1, 1.9)
    diff_gain = jnp.clip(1.0 + 0.18 * jax.random.normal(seeds[14], (HEAD,), jnp.float32), 0.1, 1.9)
    diff_lambda = jnp.clip(0.3 + 0.5 * jax.random.uniform(seeds[15], (HEADS,), jnp.float32) ** levels(seeds[15], (HEADS,), ((0, 4),), -0.2, 0.2), 0.3, 0.8)
    recur_out = normal_values(seeds[16], (HEADS * HEAD, D), (2 * HEADS * HEAD) ** -0.5, 0.125, ((0, 4),))
    diff_out = normal_values(seeds[17], (HEADS * HEAD, D), (2 * HEADS * HEAD) ** -0.5, 0.125, ((0, 4),))
    final_gain = jnp.clip(1.0 + 0.18 * jax.random.normal(seeds[18], (D,), jnp.float32), 0.1, 1.9)
    return dict(tokens=tokens, input_gain=input_gain, recur_query=recur_query, recur_forget=recur_forget, recur_input=recur_input, recur_gate=recur_gate, first_query=first_query, second_query=second_query, first_key=first_key, second_key=second_key, diff_value=diff_value, forget_floor=forget_floor, decay_shift=decay_shift, recur_gain=recur_gain, diff_gain=diff_gain, diff_lambda=diff_lambda, recur_out=recur_out, diff_out=diff_out, final_gain=final_gain)


EPSILON = 1e-06
TOP_PRECISION = lax.Precision.HIGHEST
NEGATIVE = -1e+30

def row_norm(value_rows, gain):
    mean_square = lax.optimization_barrier(jnp.mean(value_rows * value_rows, axis=-1, keepdims=True))
    return value_rows * lax.rsqrt(mean_square + EPSILON) * gain

def block_step(memory_state, inputs):
    query_vector, keyed_values, value_rows, decay = inputs
    length = query_vector.shape[1]
    running_total = jnp.cumsum(decay, axis=1)
    causal = jnp.tril(jnp.ones((length, length), bool))
    carried_state = jnp.einsum('sqr,sri->sqi', query_vector * jnp.exp(running_total), memory_state, precision=TOP_PRECISION)
    spread = running_total[:, :, None, :] - running_total[:, None, :, :]
    factors = jnp.exp(jnp.where(causal[None, :, :, None], spread, -jnp.inf))
    scores = jnp.einsum('htk,htsk,hsk->hts', query_vector, factors, keyed_values, precision=TOP_PRECISION)
    within = jnp.einsum('hts,hsv->htv', scores, value_rows, precision=TOP_PRECISION)
    final_state = running_total[:, -1]
    memory_state = jnp.exp(final_state)[:, :, None] * memory_state + jnp.einsum('ojr,ojw->orw', keyed_values * jnp.exp(final_state[:, None] - running_total), value_rows, precision=TOP_PRECISION)
    return (memory_state, carried_state + within)

def recurrence(query_vector, keyed_values, value_rows, decay):
    total = query_vector.shape[0]
    heads = query_vector.shape[1]
    blocks = total // SPAN

    def arrange(array):
        return jnp.transpose(array.reshape(blocks, SPAN, heads, array.shape[-1]), (0, 2, 1, 3))
    memory_state = jnp.zeros((heads, query_vector.shape[2], value_rows.shape[2]), jnp.float32)
    memory_state, outputs = lax.scan(block_step, memory_state, (arrange(query_vector), arrange(keyed_values), arrange(value_rows), arrange(decay)))
    return jnp.transpose(outputs, (0, 2, 1, 3)).reshape(total, heads, value_rows.shape[2])

def attend_head(inputs):
    query_one, query_two, key_one, key_two, value_rows, weight = inputs
    total = value_rows.shape[0]
    step = math.gcd(total, 512)

    def query_block(start):
        token_positions = start + jnp.arange(step).astype(jnp.int32)
        visible = token_positions[:, None] >= jnp.arange(total).astype(jnp.int32)[None, :]
        results = []
        for query_vector, keys in ((query_one, key_one), (query_two, key_two)):
            block = lax.dynamic_slice_in_dim(query_vector, start, step, 0)
            scores = jnp.dot(block, keys.T, preferred_element_type=jnp.float32) * QK ** (-0.5)
            scores = jnp.where(visible, scores, NEGATIVE)
            maxima = lax.optimization_barrier(jnp.max(scores, axis=-1))
            weights = jnp.where(visible, jnp.exp(scores - maxima[:, None]), 0.0)
            sums = lax.optimization_barrier(jnp.sum(weights, axis=-1))
            totals = jnp.dot(weights.astype(jnp.bfloat16), value_rows, preferred_element_type=jnp.float32)
            results.append((maxima + jnp.log(sums), totals / sums[:, None]))
        combined = results[0][1] - weight * results[1][1]
        return (combined, jnp.stack([results[0][0], results[1][0]]))
    starts = (jnp.arange(total // step) * step).astype(jnp.int32)
    combined, logsum = lax.map(query_block, starts)
    return (combined.reshape(total, value_rows.shape[1]), jnp.transpose(logsum, (1, 0, 2)).reshape(2, total))

def reference(tokens, input_gain, recur_query, recur_forget, recur_input, recur_gate, first_query, second_query, first_key, second_key, diff_value, forget_floor, decay_shift, recur_gain, diff_gain, diff_lambda, recur_out, diff_out, final_gain):
    total = tokens.shape[0]
    normed = row_norm(tokens.astype(jnp.float32), input_gain).astype(jnp.bfloat16)

    def project(matrix):
        return jnp.dot(normed, matrix, preferred_element_type=jnp.float32).astype(jnp.bfloat16)
    query_readout = project(recur_query).astype(jnp.float32).reshape(total, HEADS, STATE_K)
    forget_logit = project(recur_forget).astype(jnp.float32).reshape(total, HEADS, STATE_K)
    input_rows = project(recur_input).astype(jnp.float32).reshape(total, HEADS, HEAD)
    gate_rows = project(recur_gate).astype(jnp.float32)
    keyed_values = forget_floor[None] * jax.nn.sigmoid(-forget_logit)
    decay = jnp.log1p(-keyed_values) + jnp.transpose(decay_shift)[:, :, None]
    recurrent = recurrence(query_readout, keyed_values, input_rows, decay)
    recur_mix = row_norm(recurrent, recur_gain).reshape(total, HEADS * HEAD) * jax.nn.silu(gate_rows)

    def by_head(matrix, width):
        return jnp.transpose(project(matrix).reshape(total, HEADS, width), (1, 0, 2))
    combined, logsum = lax.map(attend_head, (by_head(first_query, QK), by_head(second_query, QK), by_head(first_key, QK), by_head(second_key, QK), by_head(diff_value, HEAD), diff_lambda))
    diff_mix = jnp.transpose(row_norm(combined, diff_gain), (1, 0, 2)).reshape(total, HEADS * HEAD)
    row_logsum = jnp.transpose(logsum, (1, 0, 2))
    mixed = jnp.concatenate([recur_mix, diff_mix], axis=1).astype(jnp.bfloat16)
    stacked = jnp.concatenate([recur_out, diff_out], axis=0)
    merged = jnp.dot(mixed, stacked, preferred_element_type=jnp.float32)
    layer_out = row_norm(merged, final_gain).astype(jnp.bfloat16)
    return (layer_out, row_logsum)
```

```python
import functools
import math

import jax
import jax.numpy as jnp
from jax import lax
from jax.experimental import pallas as pl
from jax.experimental.pallas import tpu as pltpu
from jax.sharding import PartitionSpec as P

SPAN = 64
EPSILON = 1e-06
NEGATIVE = -1e30
F32 = jnp.float32
BF16 = jnp.bfloat16
MESH = pl.DeviceIdType.MESH
VMEM = pl.BlockSpec(memory_space=pltpu.VMEM)
SMEM = pl.BlockSpec(memory_space=pltpu.SMEM)
ANY = pl.BlockSpec(memory_space=pl.ANY)


def params(cid):
    return pltpu.CompilerParams(
        collective_id=cid, has_side_effects=True, vmem_limit_bytes=56 * 1024 * 1024
    )


def row_norm(value_rows, gain):
    mean_square = jnp.mean(value_rows * value_rows, axis=-1, keepdims=True)
    return value_rows * lax.rsqrt(mean_square + EPSILON) * gain


def meet(axis, n):
    me = lax.axis_index(axis)
    barrier = pltpu.get_barrier_semaphore()
    for k in range(1, n):
        pl.semaphore_signal(
            barrier, inc=1, device_id={axis: lax.rem(me + k, n)}, device_id_type=MESH
        )
    pl.semaphore_wait(barrier, n - 1)


def remote(src, dst, send, recv, axis, peer):
    return pltpu.make_async_remote_copy(
        src_ref=src,
        dst_ref=dst,
        send_sem=send,
        recv_sem=recv,
        device_id={axis: peer},
        device_id_type=MESH,
    )


def dot(a, b):
    return jnp.dot(a, b, preferred_element_type=F32)


def dot_t(a, b):
    return lax.dot_general(a, b, (((1,), (1,)), ((), ())), preferred_element_type=F32)


def dot_0(a, b):
    return lax.dot_general(a, b, (((0,), (0,)), ((), ())), preferred_element_type=F32)


def project_kernel(widths, heads, fold, *refs):
    nw = len(widths)
    x_ref = refs[0]
    weights = refs[1 : 1 + nw]
    rq, rf, ri, rg, kv, qs = refs[1 + nw : 7 + nw]
    xs, wbuf, proj, wsem, ssem, rsem, lsem = refs[7 + nw :]
    rows = x_ref.shape[0]
    me = lax.axis_index("tp")
    a, c = me // 2, lax.rem(me, 2)
    far, sib = (1 - a) * 2 + c, a * 2 + (1 - c)
    offs = [sum(widths[:i]) for i in range(nw)]
    loads = [
        pltpu.make_async_copy(w, wbuf.at[:, pl.ds(o, n)], wsem.at[i])
        for i, (w, o, n) in enumerate(zip(weights, offs, widths))
    ]
    meet("tp", 4)
    pieces = 2
    part = rows // pieces
    cross = []
    for p in range(pieces):
        cp = remote(
            x_ref.at[pl.ds(p * part, part)],
            xs.at[pl.ds(me * rows + p * part, part)],
            ssem.at[p],
            rsem.at[p],
            "tp",
            far,
        )
        cp.start()
        cross.append(cp)
    side = remote(
        x_ref, xs.at[pl.ds(me * rows, rows)], ssem.at[pieces], rsem.at[pieces], "tp", sib
    )
    side.start()
    own = pltpu.make_async_copy(x_ref, xs.at[pl.ds(me * rows, rows)], lsem)
    own.start()
    for load in loads:
        load.start()
    own.wait()
    side.wait()
    for load in loads:
        load.wait()
    tile = 256
    count = sum(widths) // tile

    def group(g):
        base = pl.multiple_of(g * 2 * rows, 2 * rows)

        def one(t, _):
            cols = pl.ds(pl.multiple_of(t * tile, tile), tile)
            proj[pl.ds(base, 2 * rows), cols] = dot(
                xs[pl.ds(base, 2 * rows), :], wbuf[:, cols]
            ).astype(BF16)
            return 0

        lax.fori_loop(0, count, one, 0)

    forward = []
    for p in range(pieces):
        cross[p].wait_recv()
        where = pl.ds(far * rows + p * part, part)
        cp = remote(
            xs.at[where],
            xs.at[where],
            ssem.at[pieces + 1 + p],
            rsem.at[pieces + 1 + p],
            "tp",
            sib,
        )
        cp.start()
        forward.append(cp)
    group(a)
    for cp in forward:
        cp.wait()
    for cp in cross:
        cp.wait_send()
    group(1 - a)
    rq[...] = proj[:, offs[0] : offs[0] + widths[0]]
    rf[...] = proj[:, offs[1] : offs[1] + widths[1]]
    ri[...] = proj[:, offs[2] : offs[2] + widths[2]]
    rg[...] = proj[:, offs[3] : offs[3] + widths[3]]
    pair = widths[4] // heads
    wide = widths[8] // heads
    for h in range(heads):
        kv[h] = jnp.concatenate(
            [
                proj[:, offs[6] + h * pair : offs[6] + (h + 1) * pair],
                proj[:, offs[7] + h * pair : offs[7] + (h + 1) * pair],
                proj[:, offs[8] + h * wide : offs[8] + (h + 1) * wide],
            ],
            axis=1,
        )
        parts = []
        for j in (4, 5):
            scaled = proj[:, offs[j] + h * pair : offs[j] + (h + 1) * pair].astype(F32) * fold
            high = scaled.astype(BF16)
            parts += [high, (scaled - high.astype(F32)).astype(BF16)]
        qs[h] = jnp.concatenate(parts, axis=1)


def recur_kernel(n, heads, rq, rf, ri, kv, qs, floor, shift, *refs):
    local, qdecay, state, total, kv_all, q_all, st, ssem, rsem, lsem = refs
    me = lax.axis_index("sp")
    share = n // heads
    rows = rq.shape[0]
    mine = rows // share
    keys = floor.shape[1] // heads
    width = ri.shape[1] // heads
    meet("sp", n)
    copies = []
    for k in range(1, n):
        peer = lax.rem(me + k, n)
        head, portion = peer // share, lax.rem(peer, share)
        copies.append(
            remote(kv.at[head], kv_all.at[me], ssem.at[0, k], rsem.at[0, k], "sp", peer)
        )
        copies.append(
            remote(
                qs.at[head, pl.ds(pl.multiple_of(portion * mine, mine), mine)],
                q_all.at[me],
                ssem.at[1, k],
                rsem.at[1, k],
                "sp",
                peer,
            )
        )
    for cp in copies:
        cp.start()
    head, portion = me // share, lax.rem(me, share)
    own_kv = pltpu.make_async_copy(kv.at[head], kv_all.at[me], lsem.at[0])
    own_q = pltpu.make_async_copy(
        qs.at[head, pl.ds(pl.multiple_of(portion * mine, mine), mine)], q_all.at[me], lsem.at[1]
    )
    own_kv.start()
    own_q.start()

    st[...] = jnp.zeros_like(st)
    lower = lax.broadcasted_iota(jnp.int32, (SPAN, SPAN), 0) >= lax.broadcasted_iota(
        jnp.int32, (SPAN, SPAN), 1
    )
    ones = jnp.where(lower, 1.0, 0.0).astype(BF16)

    def chunk(i, run):
        at = pl.ds(pl.multiple_of(i * SPAN, SPAN), SPAN)
        key = floor[...] * jax.nn.sigmoid(-rf[at, :].astype(F32))
        moves = shift[at, :]
        decay = jnp.log1p(-key) + jnp.concatenate(
            [jnp.broadcast_to(moves[:, h : h + 1], (SPAN, keys)) for h in range(heads)], axis=1
        )
        high = decay.astype(BF16)
        rest = decay - high.astype(F32)
        mid = rest.astype(BF16)
        low = (rest - mid.astype(F32)).astype(BF16)
        along = dot(ones, high) + dot(ones, mid) + dot(ones, low)
        last = along[SPAN - 1 : SPAN, :]
        query = rq[at, :].astype(F32)
        scaled = query * jnp.exp(along)
        front = scaled.astype(BF16)
        qdecay[at, :] = (query * jnp.exp(along + run)).astype(BF16)
        back = (key * jnp.exp(-along)).astype(BF16)
        push = (key * jnp.exp(last - along)).astype(BF16)
        keep = jnp.exp(last)
        for h in range(heads):
            lanes = slice(h * keys, (h + 1) * keys)
            value = ri[at, h * width : (h + 1) * width]
            score = jnp.where(lower, dot_t(front[:, lanes], back[:, lanes]), 0.0)
            local[at, h * width : (h + 1) * width] = dot(score.astype(BF16), value) + dot_t(
                front[:, lanes], st[h].astype(BF16)
            )
            st[h] = keep[:, lanes] * st[h] + dot_0(value, push[:, lanes])
        return run + last

    run = lax.fori_loop(0, rows // SPAN, chunk, jnp.zeros((1, heads * keys), F32))
    state[...] = st[...].astype(BF16)
    total[...] = jnp.broadcast_to(run, total.shape)
    own_kv.wait()
    own_q.wait()
    for cp in copies:
        cp.wait()


def attend_kernel(n, heads, q_all, kv_all, state, total, lam, gain, *refs):
    msg, incoming, kd, va, states, totals, ssem, rsem = refs
    me = lax.axis_index("sp")
    share = n // heads
    portion = lax.rem(me, share)
    rows = kv_all.shape[1]
    mine = q_all.shape[1]
    width = gain.shape[1]
    pair = (kv_all.shape[2] - width) // 2
    meet("sp", n)

    def copies(k):
        peer = lax.rem(me + k, n)
        return (
            remote(state, states.at[me], ssem.at[0, k], rsem.at[0, k], "sp", peer),
            remote(total, totals.at[me], ssem.at[1, k], rsem.at[1, k], "sp", peer),
        )

    for k in range(1, n):

        @pl.when(me + k < n)
        def _():
            for cp in copies(k):
                cp.start()

    def prepare(b, _):
        block = kv_all[b]
        one, two = block[:, :pair], block[:, pair : 2 * pair]
        kd[b] = jnp.concatenate([one, one, two, two], axis=1)
        va[b] = jnp.concatenate([block[:, 2 * pair :], jnp.ones((rows, width), BF16)], axis=1)
        return 0

    lax.fori_loop(0, n, prepare, 0)
    visible = (
        portion * mine + lax.broadcasted_iota(jnp.int32, (mine, rows), 0)
    ) >= lax.broadcasted_iota(jnp.int32, (mine, rows), 1)

    def block(b, _):
        queries = [q_all[b, :, 0 : 2 * pair], q_all[b, :, 2 * pair : 4 * pair]]

        def step(u, carry, mask):
            out = []
            for j in range(2):
                top, acc = carry[2 * j], carry[2 * j + 1]
                score = dot_t(queries[j], kd[u, :, 2 * pair * j : 2 * pair * (j + 1)])
                if mask:
                    score = jnp.where(visible, score, NEGATIVE)
                newest = jnp.maximum(top, jnp.max(score, axis=1, keepdims=True))
                weight = jnp.exp2(score - newest).astype(BF16)
                out += [newest, acc * jnp.exp2(top - newest) + dot(weight, va[u])]
            return tuple(out)

        first = (
            jnp.full((mine, 1), NEGATIVE, F32),
            jnp.zeros((mine, 2 * width), F32),
        ) * 2
        carry = step(b, first, True)
        top1, acc1, top2, acc2 = lax.fori_loop(0, b, lambda u, s: step(u, s, False), carry)
        sum1, sum2 = acc1[:, width : width + 1], acc2[:, width : width + 1]
        out = acc1[:, :width] / sum1 - lam[0, 0] * (acc2[:, :width] / sum2)
        parts = [row_norm(out, gain[...]).astype(BF16)]
        for top, total_weight in ((top1, sum1), (top2, sum2)):
            value = (top + jnp.log2(total_weight)) * math.log(2.0)
            for _ in range(3):
                piece = value.astype(BF16)
                parts.append(piece)
                value = value - piece.astype(F32)
        parts.append(jnp.zeros((mine, msg.shape[2] - width - 6), BF16))
        msg[b] = jnp.concatenate(parts, axis=1)
        return 0

    lax.fori_loop(0, n, block, 0)

    for k in range(1, n):

        @pl.when(me + k < n)
        def _():
            for cp in copies(k):
                cp.wait_send()

        @pl.when(me >= k)
        def _():
            for cp in copies(k):
                cp.wait_recv()

    incoming[...] = jnp.zeros_like(incoming)
    keys = state.shape[2]

    def join(b, _):
        grow = jnp.exp(totals[b])
        for h in range(heads):
            incoming[h] = grow[0:1, h * keys : (h + 1) * keys] * incoming[h] + states[b, h].astype(
                F32
            )
        return 0

    lax.fori_loop(0, me, join, 0)


def finish_kernel(n, heads, msg, local, qdecay, incoming, gate, gain, *refs):
    mixed, logsum, back, ssem, rsem, lsem = refs
    me = lax.axis_index("sp")
    share = n // heads
    mine = msg.shape[1]
    width = gain.shape[1]
    keys = qdecay.shape[1] // heads
    meet("sp", n)
    copies = []
    for k in range(1, n):
        peer = lax.rem(me + k, n)
        copies.append(remote(msg.at[peer], back.at[me], ssem.at[k], rsem.at[k], "sp", peer))
    for cp in copies:
        cp.start()
    own = pltpu.make_async_copy(msg.at[me], back.at[me], lsem)
    own.start()
    for h in range(heads):
        lanes = slice(h * width, (h + 1) * width)
        value = local[:, lanes] + dot_t(
            qdecay[:, h * keys : (h + 1) * keys], incoming[h].astype(BF16)
        )
        mixed[:, lanes] = (row_norm(value, gain[...]) * jax.nn.silu(gate[:, lanes].astype(F32))).astype(
            BF16
        )
    own.wait()
    for cp in copies:
        cp.wait()
    for h in range(heads):
        for s in range(share):
            block = back[h * share + s]
            where = slice(s * mine, (s + 1) * mine)
            mixed[where, (heads + h) * width : (heads + h + 1) * width] = block[:, :width]
            turned = jnp.transpose(block.astype(F32))
            for j in range(2):
                at = width + 3 * j
                logsum[j, h : h + 1, where] = (
                    turned[at : at + 1] + turned[at + 1 : at + 2]
                ) + turned[at + 2 : at + 3]


def merge_kernel(n, mixed, recur, diff, gain, out, got, rbuf, dbuf, ssem, rsem, lsem):
    me = lax.axis_index("tp")
    rows = out.shape[0]
    half = mixed.shape[1] // 2
    loads = [
        pltpu.make_async_copy(recur, rbuf, lsem.at[1]),
        pltpu.make_async_copy(diff, dbuf, lsem.at[2]),
    ]
    meet("tp", n)
    copies = []
    for k in range(1, n):
        peer = lax.rem(me + k, n)
        copies.append(
            remote(
                mixed.at[pl.ds(pl.multiple_of(peer * rows, rows), rows)],
                got.at[me],
                ssem.at[k],
                rsem.at[k],
                "tp",
                peer,
            )
        )
    for cp in copies:
        cp.start()
    own = pltpu.make_async_copy(
        mixed.at[pl.ds(pl.multiple_of(me * rows, rows), rows)], got.at[me], lsem.at[0]
    )
    own.start()
    for load in loads:
        load.start()
    for load in loads:
        load.wait()
    own.wait()
    for cp in copies:
        cp.wait()
    left = jnp.concatenate([got[g, :, :half] for g in range(n)], axis=1)
    right = jnp.concatenate([got[g, :, half:] for g in range(n)], axis=1)
    merged = dot(left, rbuf[...]) + dot(right, dbuf[...])
    out[...] = row_norm(merged, gain[...]).astype(BF16)


def body(
    tokens,
    input_gain,
    recur_query,
    recur_forget,
    recur_input,
    recur_gate,
    first_query,
    second_query,
    first_key,
    second_key,
    diff_value,
    forget_floor,
    decay_shift,
    recur_gain,
    diff_gain,
    diff_lambda,
    recur_out,
    diff_out,
    final_gain,
):
    groups = lax.axis_size("tp")
    blocks = lax.axis_size("sp")
    heads, keys = forget_floor.shape
    width = recur_gain.shape[0]
    rows = decay_shift.shape[1]
    piece, model = tokens.shape
    share = blocks // heads
    mine = rows // share
    pair = first_query.shape[1] // heads
    assert groups == 4 and blocks % heads == 0 and rows % SPAN == 0
    message = 2 * pair + width
    weights = (
        recur_query,
        recur_forget,
        recur_input,
        recur_gate,
        first_query,
        second_query,
        first_key,
        second_key,
        diff_value,
    )
    widths = tuple(w.shape[1] for w in weights)
    shape = jax.ShapeDtypeStruct
    dma = pltpu.SemaphoreType.DMA
    normed = row_norm(tokens.astype(F32), input_gain).astype(BF16)
    rq, rf, ri, rg, kv, qs = pl.pallas_call(
        functools.partial(
            project_kernel, widths, heads, pair ** (-0.5) / math.log(2.0)
        ),
        out_shape=(
            shape((rows, widths[0]), BF16),
            shape((rows, widths[1]), BF16),
            shape((rows, widths[2]), BF16),
            shape((rows, widths[3]), BF16),
            shape((heads, rows, message), BF16),
            shape((heads, rows, 4 * pair), BF16),
        ),
        in_specs=[VMEM] + [ANY] * len(weights),
        out_specs=(VMEM,) * 6,
        scratch_shapes=[
            pltpu.VMEM((rows, model), BF16),
            pltpu.VMEM((model, sum(widths)), BF16),
            pltpu.VMEM((rows, sum(widths)), BF16),
            dma((len(weights),)),
            dma((5,)),
            dma((5,)),
            dma,
        ],
        compiler_params=params(0),
        name="project",
    )(normed, *weights)
    recur_out, diff_out, kv = lax.optimization_barrier((recur_out, diff_out, kv))
    full_recur = lax.all_gather(recur_out, "tp", axis=0, tiled=True)
    full_diff = lax.all_gather(diff_out, "tp", axis=0, tiled=True)
    local, qdecay, state, total, kv_all, q_all = pl.pallas_call(
        functools.partial(recur_kernel, blocks, heads),
        out_shape=(
            shape((rows, heads * width), F32),
            shape((rows, heads * keys), BF16),
            shape((heads, width, keys), BF16),
            shape((8, heads * keys), F32),
            shape((blocks, rows, message), BF16),
            shape((blocks, mine, 4 * pair), BF16),
        ),
        in_specs=[VMEM] * 7,
        out_specs=(VMEM,) * 6,
        scratch_shapes=[
            pltpu.VMEM((heads, width, keys), F32),
            dma((2, blocks)),
            dma((2, blocks)),
            dma((2,)),
        ],
        compiler_params=params(1),
        name="recur",
    )(rq, rf, ri, kv, qs, forget_floor.reshape(1, heads * keys), jnp.transpose(decay_shift))
    lam = lax.dynamic_slice_in_dim(diff_lambda, lax.axis_index("sp") // share, 1, 0)
    msg, incoming = pl.pallas_call(
        functools.partial(attend_kernel, blocks, heads),
        out_shape=(
            shape((blocks, mine, 2 * width), BF16),
            shape((heads, width, keys), F32),
        ),
        in_specs=[VMEM] * 4 + [SMEM, VMEM],
        out_specs=(VMEM,) * 2,
        scratch_shapes=[
            pltpu.VMEM((blocks, rows, 4 * pair), BF16),
            pltpu.VMEM((blocks, rows, 2 * width), BF16),
            pltpu.VMEM((blocks, heads, width, keys), BF16),
            pltpu.VMEM((blocks, 8, heads * keys), F32),
            dma((2, blocks)),
            dma((2, blocks)),
        ],
        compiler_params=params(2),
        name="attend",
    )(q_all, kv_all, state, total, lam.reshape(1, 1), diff_gain.reshape(1, width))
    mixed, logsum = pl.pallas_call(
        functools.partial(finish_kernel, blocks, heads),
        out_shape=(
            shape((rows, 2 * heads * width), BF16),
            shape((2, heads, rows), F32),
        ),
        in_specs=[VMEM] * 6,
        out_specs=(VMEM,) * 2,
        scratch_shapes=[
            pltpu.VMEM((blocks, mine, 2 * width), BF16),
            dma((blocks,)),
            dma((blocks,)),
            dma,
        ],
        compiler_params=params(3),
        name="finish",
    )(msg, local, qdecay, incoming, rg, recur_gain.reshape(1, width))
    layer_out = pl.pallas_call(
        functools.partial(merge_kernel, groups),
        out_shape=shape((piece, model), BF16),
        in_specs=[VMEM, ANY, ANY, VMEM],
        out_specs=VMEM,
        scratch_shapes=[
            pltpu.VMEM((groups, piece, 2 * heads * width), BF16),
            pltpu.VMEM(full_recur.shape, BF16),
            pltpu.VMEM(full_diff.shape, BF16),
            dma((groups,)),
            dma((groups,)),
            dma((3,)),
        ],
        compiler_params=params(4),
        name="merge",
    )(mixed, full_recur, full_diff, final_gain.reshape(1, model))
    return layer_out, logsum


def solution(mesh):
    in_specs = (
        P(("sp", "tp"), None),
        P(),
        P(None, "tp"),
        P(None, "tp"),
        P(None, "tp"),
        P(None, "tp"),
        P(None, "tp"),
        P(None, "tp"),
        P(None, "tp"),
        P(None, "tp"),
        P(None, "tp"),
        P("tp", None),
        P("tp", "sp"),
        P(),
        P(),
        P("tp"),
        P("tp", None),
        P("tp", None),
        P(),
    )
    out_specs = (P(("sp", "tp"), None), P(None, "tp", "sp"))
    return jax.shard_map(body, mesh=mesh, in_specs=in_specs, out_specs=out_specs, check_vma=False)
```

```python
import functools
import math

import jax
import jax.numpy as jnp
from jax import lax
from jax.experimental import pallas as pl
from jax.experimental.pallas import tpu as pltpu
from jax.sharding import PartitionSpec as P

SPAN = 64
EPSILON = 1e-06
NEGATIVE = -1e30
F32 = jnp.float32
BF16 = jnp.bfloat16
MESH = pl.DeviceIdType.MESH
VMEM = pl.BlockSpec(memory_space=pltpu.VMEM)
SMEM = pl.BlockSpec(memory_space=pltpu.SMEM)
ANY = pl.BlockSpec(memory_space=pl.ANY)


def params(cid):
    return pltpu.CompilerParams(
        collective_id=cid, has_side_effects=True, vmem_limit_bytes=56 * 1024 * 1024
    )


def row_norm(value_rows, gain):
    mean_square = jnp.mean(value_rows * value_rows, axis=-1, keepdims=True)
    return value_rows * lax.rsqrt(mean_square + EPSILON) * gain


def around():
    me = lax.axis_index("tp")
    a, c = me // 2, lax.rem(me, 2)
    return me, (1 - a) * 2 + c, a * 2 + (1 - c), (1 - a) * 2 + (1 - c)


def meet(axis, n, *others):
    me = lax.axis_index(axis)
    barrier = pltpu.get_barrier_semaphore()
    for k in range(1, n):
        pl.semaphore_signal(
            barrier, inc=1, device_id={axis: lax.rem(me + k, n)}, device_id_type=MESH
        )
    for other in others:
        pl.semaphore_signal(barrier, inc=1, device_id={"tp": other}, device_id_type=MESH)
    pl.semaphore_wait(barrier, n - 1 + len(others))


def remote(src, dst, send, recv, axis, peer):
    return pltpu.make_async_remote_copy(
        src_ref=src,
        dst_ref=dst,
        send_sem=send,
        recv_sem=recv,
        device_id={axis: peer},
        device_id_type=MESH,
    )


def dot(a, b):
    return jnp.dot(a, b, preferred_element_type=F32)


def dot_t(a, b):
    return lax.dot_general(a, b, (((1,), (1,)), ((), ())), preferred_element_type=F32)


def dot_0(a, b):
    return lax.dot_general(a, b, (((0,), (0,)), ((), ())), preferred_element_type=F32)


def project_kernel(widths, heads, *refs):
    nw = len(widths)
    x_ref, gain = refs[:2]
    weights = refs[2 : 2 + nw]
    rq, rf, ri, rg, kv, qs = refs[2 + nw : 8 + nw]
    xs, xn, wbuf, proj, wsem, ssem, rsem, lsem = refs[8 + nw :]
    rows = x_ref.shape[0]
    me, far, sib, _ = around()
    a = me // 2
    offs = [sum(widths[:i]) for i in range(nw)]
    loads = [
        pltpu.make_async_copy(w, wbuf.at[:, pl.ds(o, n)], wsem.at[i])
        for i, (w, o, n) in enumerate(zip(weights, offs, widths))
    ]
    own = pltpu.make_async_copy(x_ref, xs.at[pl.ds(me * rows, rows)], lsem)
    own.start()
    meet("tp", 4)
    pieces = 4
    part = rows // pieces
    cross = []
    for p in range(pieces):
        cp = remote(
            x_ref.at[pl.ds(p * part, part)],
            xs.at[pl.ds(me * rows + p * part, part)],
            ssem.at[p],
            rsem.at[p],
            "tp",
            far,
        )
        cp.start()
        cross.append(cp)
    side = remote(
        x_ref, xs.at[pl.ds(me * rows, rows)], ssem.at[pieces], rsem.at[pieces], "tp", sib
    )
    side.start()
    for load in loads:
        load.start()
    tile = 256
    count = sum(widths) // tile
    band = 2 * rows
    pair = widths[4] // heads
    wide = widths[8] // heads
    mine = 2 * qs.shape[2]
    half = mine // 2

    def normalize(g):
        def one(i, _):
            at = pl.multiple_of(g * band + i * 32, 32)
            value = xs[pl.ds(at, 32), :].astype(F32)
            xn[pl.ds(pl.multiple_of(i * 32, 32), 32), :] = row_norm(value, gain[...]).astype(BF16)
            return 0

        lax.fori_loop(0, band // 32, one, 0)

    def group(g):
        base = pl.multiple_of(g * band, band)

        def one(t, _):
            cols = pl.ds(pl.multiple_of(t * tile, tile), tile)
            proj[:, cols] = dot(xn[...], wbuf[:, cols]).astype(BF16)
            return 0

        lax.fori_loop(0, count, one, 0)
        at = pl.ds(base, band)
        for ref, k in ((rq, 0), (rf, 1), (ri, 2), (rg, 3)):
            ref[at, :] = proj[:, offs[k] : offs[k] + widths[k]]
        for h in range(heads):
            kv[h, at, :] = jnp.concatenate(
                [
                    proj[:, offs[6] + h * pair : offs[6] + (h + 1) * pair],
                    proj[:, offs[7] + h * pair : offs[7] + (h + 1) * pair],
                    proj[:, offs[8] + h * wide : offs[8] + (h + 1) * wide],
                ],
                axis=1,
            )
            for i in range(band // mine):
                parts = []
                for start in (i * mine, i * mine + half):
                    for k in (4, 5):
                        parts.append(
                            proj[
                                start : start + half,
                                offs[k] + h * pair : offs[k] + (h + 1) * pair,
                            ]
                        )
                qs[h, g * (band // mine) + i] = jnp.concatenate(parts, axis=1)

    own.wait()
    side.wait()
    normalize(a)
    for load in loads:
        load.wait()
    group(a)
    forward = []
    for p in range(pieces):
        cross[p].wait_recv()
        where = pl.ds(far * rows + p * part, part)
        cp = remote(
            xs.at[where],
            xs.at[where],
            ssem.at[pieces + 1 + p],
            rsem.at[pieces + 1 + p],
            "tp",
            sib,
        )
        cp.start()
        forward.append(cp)
    for cp in forward:
        cp.wait()
    for cp in cross:
        cp.wait_send()
    normalize(1 - a)
    group(1 - a)


def recur_kernel(n, heads, rq, rf, ri, kv, qs, floor, shift, own_r, *refs):
    local, qdecay, state, total, kv_all, q_all, far_r, st, ssem, rsem, lsem, xsem = refs
    _, far, _, _ = around()
    me = lax.axis_index("sp")
    share = n // heads
    rows = rq.shape[0]
    keys = floor.shape[1] // heads
    width = ri.shape[1] // heads
    meet("sp", n, far)
    copies = []
    for k in range(1, n):
        peer = lax.rem(me + k, n)
        head, portion = peer // share, lax.rem(peer, share)
        copies.append(
            remote(kv.at[head], kv_all.at[me], ssem.at[0, k], rsem.at[0, k], "sp", peer)
        )
        copies.append(
            remote(
                qs.at[head, portion],
                q_all.at[me],
                ssem.at[1, k],
                rsem.at[1, k],
                "sp",
                peer,
            )
        )
    copies.append(remote(own_r, far_r, xsem.at[0], xsem.at[1], "tp", far))
    for cp in copies:
        cp.start()
    head, portion = me // share, lax.rem(me, share)
    own_kv = pltpu.make_async_copy(kv.at[head], kv_all.at[me], lsem.at[0])
    own_q = pltpu.make_async_copy(qs.at[head, portion], q_all.at[me], lsem.at[1])
    own_kv.start()
    own_q.start()

    st[...] = jnp.zeros_like(st)
    lower = lax.broadcasted_iota(jnp.int32, (SPAN, SPAN), 0) >= lax.broadcasted_iota(
        jnp.int32, (SPAN, SPAN), 1
    )
    ones = jnp.where(lower, 1.0, 0.0).astype(BF16)

    def chunk(i, run):
        at = pl.ds(pl.multiple_of(i * SPAN, SPAN), SPAN)
        key = floor[...] * jax.nn.sigmoid(-rf[at, :].astype(F32))
        moves = shift[at, :]
        decay = jnp.log1p(-key) + jnp.concatenate(
            [jnp.broadcast_to(moves[:, h : h + 1], (SPAN, keys)) for h in range(heads)], axis=1
        )
        high = decay.astype(BF16)
        rest = decay - high.astype(F32)
        mid = rest.astype(BF16)
        low = (rest - mid.astype(F32)).astype(BF16)
        along = dot(ones, high) + dot(ones, mid) + dot(ones, low)
        last = along[SPAN - 1 : SPAN, :]
        query = rq[at, :].astype(F32)
        scaled = query * jnp.exp(along)
        front = scaled.astype(BF16)
        qdecay[at, :] = (query * jnp.exp(along + run)).astype(BF16)
        back = (key * jnp.exp(-along)).astype(BF16)
        push = (key * jnp.exp(last - along)).astype(BF16)
        keep = jnp.exp(last)
        for h in range(heads):
            lanes = slice(h * keys, (h + 1) * keys)
            value = ri[at, h * width : (h + 1) * width]
            score = jnp.where(lower, dot_t(front[:, lanes], back[:, lanes]), 0.0)
            local[at, h * width : (h + 1) * width] = dot(score.astype(BF16), value) + dot_t(
                front[:, lanes], st[h].astype(BF16)
            )
            st[h] = keep[:, lanes] * st[h] + dot_0(value, push[:, lanes])
        return run + last

    run = lax.fori_loop(0, rows // SPAN, chunk, jnp.zeros((1, heads * keys), F32))
    state[...] = st[...].astype(BF16)
    total[...] = jnp.broadcast_to(run, total.shape)
    own_kv.wait()
    own_q.wait()
    for cp in copies:
        cp.wait()


def attend_kernel(n, heads, fold, q_all, kv_all, state, total, lam, gain, own_r, far_r, own_d, *refs):
    msg, lmsg, incoming, sib_r, diag_r, far_d, sib_d = refs[:7]
    kt, va, sc, states, totals, ssem, rsem, xsem, ysem = refs[7:]
    me = lax.axis_index("sp")
    _, far, sib, _ = around()
    share = n // heads
    portion = lax.rem(me, share)
    rows = kv_all.shape[1]
    mine = 2 * q_all.shape[1]
    width = gain.shape[1]
    pair = (kv_all.shape[2] - width) // 2
    meet("sp", n, far, sib)

    def copies(k):
        peer = lax.rem(me + k, n)
        return (
            remote(state, states.at[me], ssem.at[0, k], rsem.at[0, k], "sp", peer),
            remote(total, totals.at[me], ssem.at[1, k], rsem.at[1, k], "sp", peer),
        )

    for k in range(1, n):

        @pl.when(me + k < n)
        def _():
            for cp in copies(k):
                cp.start()

    moves = [
        remote(own_d, far_d, xsem.at[0], ysem.at[0], "tp", far),
        remote(own_r, sib_r, xsem.at[1], ysem.at[1], "tp", sib),
        remote(far_r, diag_r, xsem.at[2], ysem.at[2], "tp", sib),
        remote(own_d, sib_d, xsem.at[3], ysem.at[3], "tp", sib),
    ]
    for cp in moves:
        cp.start()

    def prepare(b, _):
        block = kv_all[b]
        turned = jnp.transpose(block.astype(F32)).astype(BF16)
        one, two = turned[:pair], turned[pair : 2 * pair]
        kt[b] = jnp.concatenate([one, one, two, two], axis=0)
        va[b] = jnp.concatenate([block[:, 2 * pair :], jnp.ones((rows, width), BF16)], axis=1)
        return 0

    lax.fori_loop(0, n, prepare, 0)
    lanes = 128

    def block(b, _):
        packed = q_all[b]
        both = jnp.concatenate([packed[:, : 2 * pair], packed[:, 2 * pair :]], axis=0)
        scaled = both.astype(F32) * fold
        high = scaled.astype(BF16)
        low = (scaled - high.astype(F32)).astype(BF16)
        queries = [
            jnp.concatenate(
                [high[:, j * pair : (j + 1) * pair], low[:, j * pair : (j + 1) * pair]], axis=1
            )
            for j in range(2)
        ]

        def score(u, tops, mask):
            out = []
            for j in range(2):
                value = dot(queries[j], kt[u, 2 * pair * j : 2 * pair * (j + 1), :])
                if mask:
                    visible = (
                        portion * mine + lax.broadcasted_iota(jnp.int32, (mine, rows), 0)
                    ) >= lax.broadcasted_iota(jnp.int32, (mine, rows), 1)
                    value = jnp.where(visible, value, NEGATIVE)
                sc[j, u] = value
                top = tops[j]
                for i in range(rows // lanes):
                    top = jnp.maximum(top, value[:, i * lanes : (i + 1) * lanes])
                out.append(top)
            return tuple(out)

        tops = score(b, (jnp.full((mine, lanes), NEGATIVE, F32),) * 2, True)
        tops = lax.fori_loop(0, b, lambda u, t: score(u, t, False), tops)
        tops = [jnp.max(top, axis=1, keepdims=True) for top in tops]
        wide = [jnp.broadcast_to(top, (mine, lanes)) for top in tops]

        def weigh(u, accs):
            out = []
            for j in range(2):
                weight = jnp.concatenate(
                    [
                        jnp.exp2(sc[j, u, :, i * lanes : (i + 1) * lanes] - wide[j]).astype(BF16)
                        for i in range(rows // lanes)
                    ],
                    axis=1,
                )
                out.append(accs[j] + dot(weight, va[u]))
            return tuple(out)

        acc1, acc2 = lax.fori_loop(0, b + 1, weigh, (jnp.zeros((mine, 2 * width), F32),) * 2)
        sum1, sum2 = acc1[:, width : width + 1], acc2[:, width : width + 1]
        out = acc1[:, :width] / sum1 - lam[0, 0] * (acc2[:, :width] / sum2)
        out = row_norm(out, gain[...]).astype(BF16)
        msg[b] = jnp.concatenate([out[: mine // 2], out[mine // 2 :]], axis=1)
        log1 = (tops[0] + jnp.log2(sum1)) * math.log(2.0)
        log2 = (tops[1] + jnp.log2(sum2)) * math.log(2.0)
        lane = lax.broadcasted_iota(jnp.int32, (mine, lanes), 1)
        lmsg[b] = jnp.transpose(jnp.where(lane == 0, log1, log2))[:8]
        return 0

    lax.fori_loop(0, n, block, 0)

    for k in range(1, n):

        @pl.when(me + k < n)
        def _():
            for cp in copies(k):
                cp.wait_send()

        @pl.when(me >= k)
        def _():
            for cp in copies(k):
                cp.wait_recv()

    incoming[...] = jnp.zeros_like(incoming)
    keys = state.shape[2]

    def join(b, _):
        grow = jnp.exp(totals[b])
        for h in range(heads):
            incoming[h] = grow[0:1, h * keys : (h + 1) * keys] * incoming[h] + states[b, h].astype(
                F32
            )
        return 0

    lax.fori_loop(0, me, join, 0)
    for cp in moves:
        cp.wait()


def finish_kernel(n, heads, msg, lmsg, local, qdecay, incoming, gate, gain, far_d, *refs):
    mixed, logsum, diag_d, back, lback, ssem, rsem, lsem, xsem = refs
    me = lax.axis_index("sp")
    _, _, sib, _ = around()
    share = n // heads
    half = msg.shape[1]
    mine = 2 * half
    width = gain.shape[1]
    keys = qdecay.shape[1] // heads
    meet("sp", n, sib)
    copies = []
    for k in range(1, n):
        peer = lax.rem(me + k, n)
        copies.append(
            remote(msg.at[peer], back.at[me], ssem.at[0, k], rsem.at[0, k], "sp", peer)
        )
        copies.append(
            remote(lmsg.at[peer], lback.at[me], ssem.at[1, k], rsem.at[1, k], "sp", peer)
        )
    copies.append(remote(far_d, diag_d, xsem.at[0], xsem.at[1], "tp", sib))
    for cp in copies:
        cp.start()
    own = pltpu.make_async_copy(msg.at[me], back.at[me], lsem.at[0])
    own_l = pltpu.make_async_copy(lmsg.at[me], lback.at[me], lsem.at[1])
    own.start()
    own_l.start()
    for h in range(heads):
        lanes = slice(h * width, (h + 1) * width)
        value = local[:, lanes] + dot_t(
            qdecay[:, h * keys : (h + 1) * keys], incoming[h].astype(BF16)
        )
        mixed[:, lanes] = (row_norm(value, gain[...]) * jax.nn.silu(gate[:, lanes].astype(F32))).astype(
            BF16
        )
    own.wait()
    own_l.wait()
    for cp in copies:
        cp.wait()
    for h in range(heads):
        lanes = slice((heads + h) * width, (heads + h + 1) * width)
        for s in range(share):
            block = back[h * share + s]
            mixed[s * mine : s * mine + half, lanes] = block[:, :width]
            mixed[s * mine + half : (s + 1) * mine, lanes] = block[:, width:]
            for j in range(2):
                logsum[j, h : h + 1, s * mine : (s + 1) * mine] = lback[h * share + s, j : j + 1, :]


def merge_kernel(n, mixed, gain, *refs):
    sources = refs[:8]
    out, got, rbuf, dbuf, ssem, rsem, lsem, wsem = refs[8:]
    me, *rest = around()
    rows = out.shape[0]
    half = mixed.shape[1] // 2
    loads = []
    for i, source in enumerate(sources):
        place = (me, *rest)[i % 4]
        into = (rbuf, dbuf)[i // 4]
        loads.append(
            pltpu.make_async_copy(
                source, into.at[pl.ds(pl.multiple_of(place * half, half), half)], wsem.at[i]
            )
        )
    for load in loads:
        load.start()
    meet("tp", n)
    copies = []
    for k in range(1, n):
        peer = lax.rem(me + k, n)
        copies.append(
            remote(
                mixed.at[pl.ds(pl.multiple_of(peer * rows, rows), rows)],
                got.at[me],
                ssem.at[k],
                rsem.at[k],
                "tp",
                peer,
            )
        )
    for cp in copies:
        cp.start()
    own = pltpu.make_async_copy(
        mixed.at[pl.ds(pl.multiple_of(me * rows, rows), rows)], got.at[me], lsem
    )
    own.start()
    for load in loads:
        load.wait()
    own.wait()
    for cp in copies:
        cp.wait()
    left = jnp.concatenate([got[g, :, :half] for g in range(n)], axis=1)
    right = jnp.concatenate([got[g, :, half:] for g in range(n)], axis=1)
    merged = dot(left, rbuf[...]) + dot(right, dbuf[...])
    out[...] = row_norm(merged, gain[...]).astype(BF16)


def body(
    tokens,
    input_gain,
    recur_query,
    recur_forget,
    recur_input,
    recur_gate,
    first_query,
    second_query,
    first_key,
    second_key,
    diff_value,
    forget_floor,
    decay_shift,
    recur_gain,
    diff_gain,
    diff_lambda,
    recur_out,
    diff_out,
    final_gain,
):
    groups = lax.axis_size("tp")
    blocks = lax.axis_size("sp")
    heads, keys = forget_floor.shape
    width = recur_gain.shape[0]
    rows = decay_shift.shape[1]
    piece, model = tokens.shape
    share = blocks // heads
    mine = rows // share
    pair = first_query.shape[1] // heads
    assert groups == 4 and blocks % heads == 0 and rows % SPAN == 0
    message = 2 * pair + width
    weights = (
        recur_query,
        recur_forget,
        recur_input,
        recur_gate,
        first_query,
        second_query,
        first_key,
        second_key,
        diff_value,
    )
    widths = tuple(w.shape[1] for w in weights)
    shape = jax.ShapeDtypeStruct
    dma = pltpu.SemaphoreType.DMA
    rq, rf, ri, rg, kv, qs = pl.pallas_call(
        functools.partial(project_kernel, widths, heads),
        out_shape=(
            shape((rows, widths[0]), BF16),
            shape((rows, widths[1]), BF16),
            shape((rows, widths[2]), BF16),
            shape((rows, widths[3]), BF16),
            shape((heads, rows, message), BF16),
            shape((heads, share, mine // 2, 4 * pair), BF16),
        ),
        in_specs=[ANY, VMEM] + [ANY] * len(weights),
        out_specs=(VMEM,) * 6,
        scratch_shapes=[
            pltpu.VMEM((rows, model), BF16),
            pltpu.VMEM((2 * piece, model), BF16),
            pltpu.VMEM((model, sum(widths)), BF16),
            pltpu.VMEM((2 * piece, sum(widths)), BF16),
            dma((len(weights),)),
            dma((9,)),
            dma((9,)),
            dma,
        ],
        compiler_params=params(0),
        name="project",
    )(tokens, input_gain.reshape(1, model), *weights)
    local, qdecay, state, total, kv_all, q_all, far_r = pl.pallas_call(
        functools.partial(recur_kernel, blocks, heads),
        out_shape=(
            shape((rows, heads * width), F32),
            shape((rows, heads * keys), BF16),
            shape((heads, width, keys), BF16),
            shape((8, heads * keys), F32),
            shape((blocks, rows, message), BF16),
            shape((blocks, mine // 2, 4 * pair), BF16),
            shape(recur_out.shape, BF16),
        ),
        in_specs=[VMEM] * 7 + [ANY],
        out_specs=(VMEM,) * 6 + (ANY,),
        scratch_shapes=[
            pltpu.VMEM((heads, width, keys), F32),
            dma((2, blocks)),
            dma((2, blocks)),
            dma((2,)),
            dma((2,)),
        ],
        compiler_params=params(1),
        name="recur",
    )(
        rq,
        rf,
        ri,
        kv,
        qs,
        forget_floor.reshape(1, heads * keys),
        jnp.transpose(decay_shift),
        recur_out,
    )
    lam = lax.dynamic_slice_in_dim(diff_lambda, lax.axis_index("sp") // share, 1, 0)
    msg, lmsg, incoming, sib_r, diag_r, far_d, sib_d = pl.pallas_call(
        functools.partial(attend_kernel, blocks, heads, pair ** (-0.5) / math.log(2.0)),
        out_shape=(
            shape((blocks, mine // 2, 2 * width), BF16),
            shape((blocks, 8, mine), F32),
            shape((heads, width, keys), F32),
        )
        + (shape(recur_out.shape, BF16),) * 4,
        in_specs=[VMEM] * 4 + [SMEM, VMEM] + [ANY] * 3,
        out_specs=(VMEM,) * 3 + (ANY,) * 4,
        scratch_shapes=[
            pltpu.VMEM((blocks, 4 * pair, rows), BF16),
            pltpu.VMEM((blocks, rows, 2 * width), BF16),
            pltpu.VMEM((2, blocks, mine, rows), F32),
            pltpu.VMEM((blocks, heads, width, keys), BF16),
            pltpu.VMEM((blocks, 8, heads * keys), F32),
            dma((2, blocks)),
            dma((2, blocks)),
            dma((4,)),
            dma((4,)),
        ],
        compiler_params=params(2),
        name="attend",
    )(
        q_all,
        kv_all,
        state,
        total,
        lam.reshape(1, 1),
        diff_gain.reshape(1, width),
        recur_out,
        far_r,
        diff_out,
    )
    mixed, logsum, diag_d = pl.pallas_call(
        functools.partial(finish_kernel, blocks, heads),
        out_shape=(
            shape((rows, 2 * heads * width), BF16),
            shape((2, heads, rows), F32),
            shape(diff_out.shape, BF16),
        ),
        in_specs=[VMEM] * 7 + [ANY],
        out_specs=(VMEM,) * 2 + (ANY,),
        scratch_shapes=[
            pltpu.VMEM((blocks, mine // 2, 2 * width), BF16),
            pltpu.VMEM((blocks, 8, mine), F32),
            dma((2, blocks)),
            dma((2, blocks)),
            dma((2,)),
            dma((2,)),
        ],
        compiler_params=params(3),
        name="finish",
    )(msg, lmsg, local, qdecay, incoming, rg, recur_gain.reshape(1, width), far_d)
    full = shape((groups * heads * width, model), BF16)
    layer_out = pl.pallas_call(
        functools.partial(merge_kernel, groups),
        out_shape=shape((piece, model), BF16),
        in_specs=[VMEM, VMEM] + [ANY] * 8,
        out_specs=VMEM,
        scratch_shapes=[
            pltpu.VMEM((groups, piece, 2 * heads * width), BF16),
            pltpu.VMEM(full.shape, BF16),
            pltpu.VMEM(full.shape, BF16),
            dma((groups,)),
            dma((groups,)),
            dma,
            dma((8,)),
        ],
        compiler_params=params(4),
        name="merge",
    )(
        mixed,
        final_gain.reshape(1, model),
        recur_out,
        far_r,
        sib_r,
        diag_r,
        diff_out,
        far_d,
        sib_d,
        diag_d,
    )
    return layer_out, logsum


def solution(mesh):
    in_specs = (
        P(("sp", "tp"), None),
        P(),
        P(None, "tp"),
        P(None, "tp"),
        P(None, "tp"),
        P(None, "tp"),
        P(None, "tp"),
        P(None, "tp"),
        P(None, "tp"),
        P(None, "tp"),
        P(None, "tp"),
        P("tp", None),
        P("tp", "sp"),
        P(),
        P(),
        P("tp"),
        P("tp", None),
        P("tp", None),
        P(),
    )
    out_specs = (P(("sp", "tp"), None), P(None, "tp", "sp"))
    return jax.shard_map(body, mesh=mesh, in_specs=in_specs, out_specs=out_specs, check_vma=False)
```

```python
import functools
import math

import jax
import jax.numpy as jnp
from jax import lax
from jax.experimental import pallas as pl
from jax.experimental.pallas import tpu as pltpu
from jax.sharding import PartitionSpec as P

SPAN = 64
EPSILON = 1e-06
NEGATIVE = -1e30
F32 = jnp.float32
BF16 = jnp.bfloat16
MESH = pl.DeviceIdType.MESH
VMEM = pl.BlockSpec(memory_space=pltpu.VMEM)
SMEM = pl.BlockSpec(memory_space=pltpu.SMEM)
ANY = pl.BlockSpec(memory_space=pl.ANY)


def params(cid):
    return pltpu.CompilerParams(
        collective_id=cid, has_side_effects=True, vmem_limit_bytes=56 * 1024 * 1024
    )


def row_norm(value_rows, gain):
    mean_square = jnp.mean(value_rows * value_rows, axis=-1, keepdims=True)
    return value_rows * lax.rsqrt(mean_square + EPSILON) * gain


def around():
    me = lax.axis_index("tp")
    a, c = me // 2, lax.rem(me, 2)
    return me, (1 - a) * 2 + c, a * 2 + (1 - c), (1 - a) * 2 + (1 - c)


def meet(axis, n, *others):
    me = lax.axis_index(axis)
    barrier = pltpu.get_barrier_semaphore()
    for k in range(1, n):
        pl.semaphore_signal(
            barrier, inc=1, device_id={axis: lax.rem(me + k, n)}, device_id_type=MESH
        )
    for other in others:
        pl.semaphore_signal(barrier, inc=1, device_id={"tp": other}, device_id_type=MESH)
    pl.semaphore_wait(barrier, n - 1 + len(others))


def remote(src, dst, send, recv, axis, peer):
    return pltpu.make_async_remote_copy(
        src_ref=src,
        dst_ref=dst,
        send_sem=send,
        recv_sem=recv,
        device_id={axis: peer},
        device_id_type=MESH,
    )


def dot(a, b):
    return jnp.dot(a, b, preferred_element_type=F32)


def dot_t(a, b):
    return lax.dot_general(a, b, (((1,), (1,)), ((), ())), preferred_element_type=F32)


def dot_0(a, b):
    return lax.dot_general(a, b, (((0,), (0,)), ((), ())), preferred_element_type=F32)


def project_kernel(widths, heads, *refs):
    nw = len(widths)
    x_ref, gain = refs[:2]
    weights = refs[2 : 2 + nw]
    rq, rf, ri, rg, kv, qs = refs[2 + nw : 8 + nw]
    xs, xn, wbuf, proj, wsem, ssem, rsem, lsem = refs[8 + nw :]
    rows = x_ref.shape[0]
    me, far, sib, _ = around()
    a = me // 2
    offs = [sum(widths[:i]) for i in range(nw)]
    loads = [
        pltpu.make_async_copy(w, wbuf.at[:, pl.ds(o, n)], wsem.at[i])
        for i, (w, o, n) in enumerate(zip(weights, offs, widths))
    ]
    own = pltpu.make_async_copy(x_ref, xs.at[pl.ds(me * rows, rows)], lsem)
    own.start()
    meet("tp", 4)
    pieces = 4
    part = rows // pieces
    cross = []
    for p in range(pieces):
        cp = remote(
            x_ref.at[pl.ds(p * part, part)],
            xs.at[pl.ds(me * rows + p * part, part)],
            ssem.at[p],
            rsem.at[p],
            "tp",
            far,
        )
        cp.start()
        cross.append(cp)
    side = remote(
        x_ref, xs.at[pl.ds(me * rows, rows)], ssem.at[pieces], rsem.at[pieces], "tp", sib
    )
    side.start()
    for load in loads:
        load.start()
    tile = 256
    count = sum(widths) // tile
    band = 2 * rows
    pair = widths[4] // heads
    wide = widths[8] // heads
    mine = 2 * qs.shape[2]
    half = mine // 2

    def normalize(g):
        def one(i, _):
            at = pl.multiple_of(g * band + i * 32, 32)
            value = xs[pl.ds(at, 32), :].astype(F32)
            xn[pl.ds(pl.multiple_of(i * 32, 32), 32), :] = row_norm(value, gain[...]).astype(BF16)
            return 0

        lax.fori_loop(0, band // 32, one, 0)

    def group(g):
        base = pl.multiple_of(g * band, band)

        def one(t, _):
            cols = pl.ds(pl.multiple_of(t * tile, tile), tile)
            proj[:, cols] = dot(xn[...], wbuf[:, cols]).astype(BF16)
            return 0

        lax.fori_loop(0, count, one, 0)
        at = pl.ds(base, band)
        for ref, k in ((rq, 0), (rf, 1), (ri, 2), (rg, 3)):
            ref[at, :] = proj[:, offs[k] : offs[k] + widths[k]]
        for h in range(heads):
            kv[h, at, :] = jnp.concatenate(
                [
                    proj[:, offs[6] + h * pair : offs[6] + (h + 1) * pair],
                    proj[:, offs[7] + h * pair : offs[7] + (h + 1) * pair],
                    proj[:, offs[8] + h * wide : offs[8] + (h + 1) * wide],
                ],
                axis=1,
            )
            for i in range(band // mine):
                parts = []
                for start in (i * mine, i * mine + half):
                    for k in (4, 5):
                        parts.append(
                            proj[
                                start : start + half,
                                offs[k] + h * pair : offs[k] + (h + 1) * pair,
                            ]
                        )
                qs[h, g * (band // mine) + i] = jnp.concatenate(parts, axis=1)

    own.wait()
    side.wait()
    normalize(a)
    for load in loads:
        load.wait()
    group(a)
    forward = []
    for p in range(pieces):
        cross[p].wait_recv()
        where = pl.ds(far * rows + p * part, part)
        cp = remote(
            xs.at[where],
            xs.at[where],
            ssem.at[pieces + 1 + p],
            rsem.at[pieces + 1 + p],
            "tp",
            sib,
        )
        cp.start()
        forward.append(cp)
    for cp in forward:
        cp.wait()
    for cp in cross:
        cp.wait_send()
    normalize(1 - a)
    group(1 - a)


def recur_kernel(n, heads, rq, rf, ri, kv, qs, floor, shift, own_r, *refs):
    local, qdecay, state, total, kv_all, q_all, far_r = refs[:7]
    st, turned, ssem, rsem, fsem, gsem, lsem, xsem = refs[7:]
    _, far, _, _ = around()
    me = lax.axis_index("sp")
    share = n // heads
    rows = rq.shape[0]
    keys = floor.shape[1] // heads
    width = ri.shape[1] // heads
    head, portion = me // share, lax.rem(me, share)
    meet("sp", n, far)
    direct = []
    for k in range(1, heads):
        other = lax.rem(head + k, heads)
        direct.append(
            remote(
                kv.at[other],
                kv_all.at[me],
                ssem.at[0, k],
                rsem.at[0, k],
                "sp",
                other * share + portion,
            )
        )
    copies = []
    for k in range(1, n):
        peer = lax.rem(me + k, n)
        copies.append(
            remote(
                qs.at[peer // share, lax.rem(peer, share)],
                q_all.at[me],
                ssem.at[1, k],
                rsem.at[1, k],
                "sp",
                peer,
            )
        )

    def forward(k):
        source = lax.rem(head + heads - k, heads) * share + portion
        block = kv.at[head] if k == 0 else kv_all.at[source]
        return [
            remote(
                block,
                kv_all.at[source],
                fsem.at[k, j],
                gsem.at[k, j],
                "sp",
                head * share + lax.rem(portion + j, share),
            )
            for j in range(1, share)
        ]

    for cp in direct:
        cp.start()
    forwards = forward(0)
    for cp in forwards:
        cp.start()
    copies.append(remote(own_r, far_r, xsem.at[0], xsem.at[1], "tp", far))
    for cp in copies:
        cp.start()
    own_kv = pltpu.make_async_copy(kv.at[head], kv_all.at[me], lsem.at[0])
    own_q = pltpu.make_async_copy(qs.at[head, portion], q_all.at[me], lsem.at[1])
    own_kv.start()
    own_q.start()
    turned[...] = jnp.transpose(
        jnp.concatenate([shift[...], jnp.zeros((128 - heads, rows), F32)], axis=0)
    )

    st[...] = jnp.zeros_like(st)
    lower = lax.broadcasted_iota(jnp.int32, (SPAN, SPAN), 0) >= lax.broadcasted_iota(
        jnp.int32, (SPAN, SPAN), 1
    )
    ones = jnp.where(lower, 1.0, 0.0).astype(BF16)

    def chunk(i, run):
        at = pl.ds(pl.multiple_of(i * SPAN, SPAN), SPAN)
        key = floor[...] * jax.nn.sigmoid(-rf[at, :].astype(F32))
        moves = turned[at, :]
        decay = jnp.log1p(-key) + jnp.concatenate(
            [jnp.broadcast_to(moves[:, h : h + 1], (SPAN, keys)) for h in range(heads)], axis=1
        )
        high = decay.astype(BF16)
        rest = decay - high.astype(F32)
        mid = rest.astype(BF16)
        low = (rest - mid.astype(F32)).astype(BF16)
        along = dot(ones, high) + dot(ones, mid) + dot(ones, low)
        last = along[SPAN - 1 : SPAN, :]
        query = rq[at, :].astype(F32)
        scaled = query * jnp.exp(along)
        front = scaled.astype(BF16)
        qdecay[at, :] = (query * jnp.exp(along + run)).astype(BF16)
        back = (key * jnp.exp(-along)).astype(BF16)
        push = (key * jnp.exp(last - along)).astype(BF16)
        keep = jnp.exp(last)
        for h in range(heads):
            lanes = slice(h * keys, (h + 1) * keys)
            value = ri[at, h * width : (h + 1) * width]
            score = jnp.where(lower, dot_t(front[:, lanes], back[:, lanes]), 0.0)
            local[at, h * width : (h + 1) * width] = dot(score.astype(BF16), value) + dot_t(
                front[:, lanes], st[h].astype(BF16)
            )
            st[h] = keep[:, lanes] * st[h] + dot_0(value, push[:, lanes])
        return run + last

    run = lax.fori_loop(0, rows // SPAN, chunk, jnp.zeros((1, heads * keys), F32))
    state[...] = st[...].astype(BF16)
    total[...] = jnp.broadcast_to(run, total.shape)
    for k in range(1, heads):
        direct[k - 1].wait_recv()
        for cp in forward(k):
            cp.start()
    own_kv.wait()
    own_q.wait()
    for cp in direct:
        cp.wait_send()
    for k in range(heads):
        for cp in forward(k):
            cp.wait()
    for cp in copies:
        cp.wait()


def attend_kernel(n, heads, fold, q_all, kv_all, state, total, lam, gain, own_r, far_r, own_d, *refs):
    msg, lmsg, incoming, sib_r, diag_r, far_d, sib_d = refs[:7]
    kt, va, sc, states, totals, ssem, rsem, xsem, ysem = refs[7:]
    me = lax.axis_index("sp")
    _, far, sib, _ = around()
    share = n // heads
    portion = lax.rem(me, share)
    rows = kv_all.shape[1]
    mine = 2 * q_all.shape[1]
    width = gain.shape[1]
    pair = (kv_all.shape[2] - width) // 2
    meet("sp", n, far, sib)

    def copies(k):
        peer = lax.rem(me + k, n)
        return (
            remote(state, states.at[me], ssem.at[0, k], rsem.at[0, k], "sp", peer),
            remote(total, totals.at[me], ssem.at[1, k], rsem.at[1, k], "sp", peer),
        )

    for k in range(1, n):

        @pl.when(me + k < n)
        def _():
            for cp in copies(k):
                cp.start()

    moves = [
        remote(own_d, far_d, xsem.at[0], ysem.at[0], "tp", far),
        remote(own_r, sib_r, xsem.at[1], ysem.at[1], "tp", sib),
        remote(far_r, diag_r, xsem.at[2], ysem.at[2], "tp", sib),
        remote(own_d, sib_d, xsem.at[3], ysem.at[3], "tp", sib),
    ]
    for cp in moves:
        cp.start()

    def prepare(b, _):
        block = kv_all[b]
        turned = jnp.transpose(block.astype(F32)).astype(BF16)
        one, two = turned[:pair], turned[pair : 2 * pair]
        kt[b] = jnp.concatenate([one, one, two, two], axis=0)
        va[b] = jnp.concatenate([block[:, 2 * pair :], jnp.ones((rows, width), BF16)], axis=1)
        return 0

    lax.fori_loop(0, n, prepare, 0)
    lanes = 128

    def block(b, _):
        packed = q_all[b]
        both = jnp.concatenate([packed[:, : 2 * pair], packed[:, 2 * pair :]], axis=0)
        scaled = both.astype(F32) * fold
        high = scaled.astype(BF16)
        low = (scaled - high.astype(F32)).astype(BF16)
        queries = [
            jnp.concatenate(
                [high[:, j * pair : (j + 1) * pair], low[:, j * pair : (j + 1) * pair]], axis=1
            )
            for j in range(2)
        ]

        def score(u, tops, mask):
            out = []
            for j in range(2):
                value = dot(queries[j], kt[u, 2 * pair * j : 2 * pair * (j + 1), :])
                if mask:
                    visible = (
                        portion * mine + lax.broadcasted_iota(jnp.int32, (mine, rows), 0)
                    ) >= lax.broadcasted_iota(jnp.int32, (mine, rows), 1)
                    value = jnp.where(visible, value, NEGATIVE)
                sc[j, u] = value
                top = tops[j]
                for i in range(rows // lanes):
                    top = jnp.maximum(top, value[:, i * lanes : (i + 1) * lanes])
                out.append(top)
            return tuple(out)

        tops = score(b, (jnp.full((mine, lanes), NEGATIVE, F32),) * 2, True)
        tops = lax.fori_loop(0, b, lambda u, t: score(u, t, False), tops)
        tops = [jnp.max(top, axis=1, keepdims=True) for top in tops]
        wide = [jnp.broadcast_to(top, (mine, lanes)) for top in tops]

        def weigh(u, accs):
            out = []
            for j in range(2):
                weight = jnp.concatenate(
                    [
                        jnp.exp2(sc[j, u, :, i * lanes : (i + 1) * lanes] - wide[j]).astype(BF16)
                        for i in range(rows // lanes)
                    ],
                    axis=1,
                )
                out.append(accs[j] + dot(weight, va[u]))
            return tuple(out)

        acc1, acc2 = lax.fori_loop(0, b + 1, weigh, (jnp.zeros((mine, 2 * width), F32),) * 2)
        sum1, sum2 = acc1[:, width : width + 1], acc2[:, width : width + 1]
        out = acc1[:, :width] / sum1 - lam[me // share] * (acc2[:, :width] / sum2)
        out = row_norm(out, gain[...]).astype(BF16)
        msg[b] = jnp.concatenate([out[: mine // 2], out[mine // 2 :]], axis=1)
        log1 = (tops[0] + jnp.log2(sum1)) * math.log(2.0)
        log2 = (tops[1] + jnp.log2(sum2)) * math.log(2.0)
        lane = lax.broadcasted_iota(jnp.int32, (mine, lanes), 1)
        lmsg[b] = jnp.transpose(jnp.where(lane == 0, log1, log2))[:8]
        return 0

    lax.fori_loop(0, n, block, 0)

    for k in range(1, n):

        @pl.when(me + k < n)
        def _():
            for cp in copies(k):
                cp.wait_send()

        @pl.when(me >= k)
        def _():
            for cp in copies(k):
                cp.wait_recv()

    incoming[...] = jnp.zeros_like(incoming)
    keys = state.shape[2]

    def join(b, _):
        grow = jnp.exp(totals[b])
        for h in range(heads):
            incoming[h] = grow[0:1, h * keys : (h + 1) * keys] * incoming[h] + states[b, h].astype(
                F32
            )
        return 0

    lax.fori_loop(0, me, join, 0)
    for cp in moves:
        cp.wait()


def finish_kernel(n, heads, msg, lmsg, local, qdecay, incoming, gate, gain, far_d, *refs):
    mixed, logsum, diag_d, back, lback, ssem, rsem, lsem, xsem = refs
    me = lax.axis_index("sp")
    _, _, sib, _ = around()
    share = n // heads
    half = msg.shape[1]
    mine = 2 * half
    width = gain.shape[1]
    keys = qdecay.shape[1] // heads
    meet("sp", n, sib)
    copies = []
    for k in range(1, n):
        peer = lax.rem(me + k, n)
        copies.append(
            remote(msg.at[peer], back.at[me], ssem.at[0, k], rsem.at[0, k], "sp", peer)
        )
        copies.append(
            remote(lmsg.at[peer], lback.at[me], ssem.at[1, k], rsem.at[1, k], "sp", peer)
        )
    copies.append(remote(far_d, diag_d, xsem.at[0], xsem.at[1], "tp", sib))
    for cp in copies:
        cp.start()
    own = pltpu.make_async_copy(msg.at[me], back.at[me], lsem.at[0])
    own_l = pltpu.make_async_copy(lmsg.at[me], lback.at[me], lsem.at[1])
    own.start()
    own_l.start()
    for h in range(heads):
        lanes = slice(h * width, (h + 1) * width)
        value = local[:, lanes] + dot_t(
            qdecay[:, h * keys : (h + 1) * keys], incoming[h].astype(BF16)
        )
        mixed[:, lanes] = (row_norm(value, gain[...]) * jax.nn.silu(gate[:, lanes].astype(F32))).astype(
            BF16
        )
    own.wait()
    own_l.wait()
    for cp in copies:
        cp.wait()
    for h in range(heads):
        lanes = slice((heads + h) * width, (heads + h + 1) * width)
        for s in range(share):
            block = back[h * share + s]
            mixed[s * mine : s * mine + half, lanes] = block[:, :width]
            mixed[s * mine + half : (s + 1) * mine, lanes] = block[:, width:]
            for j in range(2):
                logsum[j, h : h + 1, s * mine : (s + 1) * mine] = lback[h * share + s, j : j + 1, :]


def merge_kernel(n, mixed, gain, *refs):
    sources = refs[:8]
    out, got, rbuf, dbuf, ssem, rsem, lsem, wsem = refs[8:]
    me, *rest = around()
    rows = out.shape[0]
    half = mixed.shape[1] // 2
    loads = []
    for i, source in enumerate(sources):
        place = (me, *rest)[i % 4]
        into = (rbuf, dbuf)[i // 4]
        loads.append(
            pltpu.make_async_copy(
                source, into.at[pl.ds(pl.multiple_of(place * half, half), half)], wsem.at[i]
            )
        )
    for load in loads:
        load.start()
    meet("tp", n)
    copies = []
    for k in range(1, n):
        peer = lax.rem(me + k, n)
        copies.append(
            remote(
                mixed.at[pl.ds(pl.multiple_of(peer * rows, rows), rows)],
                got.at[me],
                ssem.at[k],
                rsem.at[k],
                "tp",
                peer,
            )
        )
    for cp in copies:
        cp.start()
    own = pltpu.make_async_copy(
        mixed.at[pl.ds(pl.multiple_of(me * rows, rows), rows)], got.at[me], lsem
    )
    own.start()
    for load in loads:
        load.wait()
    own.wait()
    for cp in copies:
        cp.wait()
    left = jnp.concatenate([got[g, :, :half] for g in range(n)], axis=1)
    right = jnp.concatenate([got[g, :, half:] for g in range(n)], axis=1)
    merged = dot(left, rbuf[...]) + dot(right, dbuf[...])
    out[...] = row_norm(merged, gain[...]).astype(BF16)


def body(
    tokens,
    input_gain,
    recur_query,
    recur_forget,
    recur_input,
    recur_gate,
    first_query,
    second_query,
    first_key,
    second_key,
    diff_value,
    forget_floor,
    decay_shift,
    recur_gain,
    diff_gain,
    diff_lambda,
    recur_out,
    diff_out,
    final_gain,
):
    groups = lax.axis_size("tp")
    blocks = lax.axis_size("sp")
    heads, keys = forget_floor.shape
    width = recur_gain.shape[0]
    rows = decay_shift.shape[1]
    piece, model = tokens.shape
    share = blocks // heads
    mine = rows // share
    pair = first_query.shape[1] // heads
    assert groups == 4 and blocks % heads == 0 and rows % SPAN == 0
    message = 2 * pair + width
    weights = (
        recur_query,
        recur_forget,
        recur_input,
        recur_gate,
        first_query,
        second_query,
        first_key,
        second_key,
        diff_value,
    )
    widths = tuple(w.shape[1] for w in weights)
    shape = jax.ShapeDtypeStruct
    dma = pltpu.SemaphoreType.DMA
    rq, rf, ri, rg, kv, qs = pl.pallas_call(
        functools.partial(project_kernel, widths, heads),
        out_shape=(
            shape((rows, widths[0]), BF16),
            shape((rows, widths[1]), BF16),
            shape((rows, widths[2]), BF16),
            shape((rows, widths[3]), BF16),
            shape((heads, rows, message), BF16),
            shape((heads, share, mine // 2, 4 * pair), BF16),
        ),
        in_specs=[ANY, VMEM] + [ANY] * len(weights),
        out_specs=(VMEM,) * 6,
        scratch_shapes=[
            pltpu.VMEM((rows, model), BF16),
            pltpu.VMEM((2 * piece, model), BF16),
            pltpu.VMEM((model, sum(widths)), BF16),
            pltpu.VMEM((2 * piece, sum(widths)), BF16),
            dma((len(weights),)),
            dma((9,)),
            dma((9,)),
            dma,
        ],
        compiler_params=params(0),
        name="project",
    )(tokens, input_gain.reshape(1, model), *weights)
    local, qdecay, state, total, kv_all, q_all, far_r = pl.pallas_call(
        functools.partial(recur_kernel, blocks, heads),
        out_shape=(
            shape((rows, heads * width), F32),
            shape((rows, heads * keys), BF16),
            shape((heads, width, keys), BF16),
            shape((8, heads * keys), F32),
            shape((blocks, rows, message), BF16),
            shape((blocks, mine // 2, 4 * pair), BF16),
            shape(recur_out.shape, BF16),
        ),
        in_specs=[VMEM] * 7 + [ANY],
        out_specs=(VMEM,) * 6 + (ANY,),
        scratch_shapes=[
            pltpu.VMEM((heads, width, keys), F32),
            pltpu.VMEM((rows, 128), F32),
            dma((2, blocks)),
            dma((2, blocks)),
            dma((heads, share)),
            dma((heads, share)),
            dma((2,)),
            dma((2,)),
        ],
        compiler_params=params(1),
        name="recur",
    )(
        rq,
        rf,
        ri,
        kv,
        qs,
        forget_floor.reshape(1, heads * keys),
        decay_shift,
        recur_out,
    )
    msg, lmsg, incoming, sib_r, diag_r, far_d, sib_d = pl.pallas_call(
        functools.partial(attend_kernel, blocks, heads, pair ** (-0.5) / math.log(2.0)),
        out_shape=(
            shape((blocks, mine // 2, 2 * width), BF16),
            shape((blocks, 8, mine), F32),
            shape((heads, width, keys), F32),
        )
        + (shape(recur_out.shape, BF16),) * 4,
        in_specs=[VMEM] * 4 + [SMEM, VMEM] + [ANY] * 3,
        out_specs=(VMEM,) * 3 + (ANY,) * 4,
        scratch_shapes=[
            pltpu.VMEM((blocks, 4 * pair, rows), BF16),
            pltpu.VMEM((blocks, rows, 2 * width), BF16),
            pltpu.VMEM((2, blocks, mine, rows), F32),
            pltpu.VMEM((blocks, heads, width, keys), BF16),
            pltpu.VMEM((blocks, 8, heads * keys), F32),
            dma((2, blocks)),
            dma((2, blocks)),
            dma((4,)),
            dma((4,)),
        ],
        compiler_params=params(2),
        name="attend",
    )(
        q_all,
        kv_all,
        state,
        total,
        diff_lambda,
        diff_gain.reshape(1, width),
        recur_out,
        far_r,
        diff_out,
    )
    mixed, logsum, diag_d = pl.pallas_call(
        functools.partial(finish_kernel, blocks, heads),
        out_shape=(
            shape((rows, 2 * heads * width), BF16),
            shape((2, heads, rows), F32),
            shape(diff_out.shape, BF16),
        ),
        in_specs=[VMEM] * 7 + [ANY],
        out_specs=(VMEM,) * 2 + (ANY,),
        scratch_shapes=[
            pltpu.VMEM((blocks, mine // 2, 2 * width), BF16),
            pltpu.VMEM((blocks, 8, mine), F32),
            dma((2, blocks)),
            dma((2, blocks)),
            dma((2,)),
            dma((2,)),
        ],
        compiler_params=params(3),
        name="finish",
    )(msg, lmsg, local, qdecay, incoming, rg, recur_gain.reshape(1, width), far_d)
    full = shape((groups * heads * width, model), BF16)
    layer_out = pl.pallas_call(
        functools.partial(merge_kernel, groups),
        out_shape=shape((piece, model), BF16),
        in_specs=[VMEM, VMEM] + [ANY] * 8,
        out_specs=VMEM,
        scratch_shapes=[
            pltpu.VMEM((groups, piece, 2 * heads * width), BF16),
            pltpu.VMEM(full.shape, BF16),
            pltpu.VMEM(full.shape, BF16),
            dma((groups,)),
            dma((groups,)),
            dma,
            dma((8,)),
        ],
        compiler_params=params(4),
        name="merge",
    )(
        mixed,
        final_gain.reshape(1, model),
        recur_out,
        far_r,
        sib_r,
        diag_r,
        diff_out,
        far_d,
        sib_d,
        diag_d,
    )
    return layer_out, logsum


def solution(mesh):
    in_specs = (
        P(("sp", "tp"), None),
        P(),
        P(None, "tp"),
        P(None, "tp"),
        P(None, "tp"),
        P(None, "tp"),
        P(None, "tp"),
        P(None, "tp"),
        P(None, "tp"),
        P(None, "tp"),
        P(None, "tp"),
        P("tp", None),
        P("tp", "sp"),
        P(),
        P(),
        P("tp"),
        P("tp", None),
        P("tp", None),
        P(),
    )
    out_specs = (P(("sp", "tp"), None), P(None, "tp", "sp"))
    return jax.shard_map(body, mesh=mesh, in_specs=in_specs, out_specs=out_specs, check_vma=False)
```
